32 devices in a mesh: rep: 2 (over x), fs: 8 (over z, y), tp: 2 (over core).
Axes of the slice: x: 2, y: 2, z: 4, core: 2. Of those that a mesh axis runs over, the one named last changes fastest.
Arguments:
- tokens: bfloat16 [6144, 2048], P(('rep', 'fs'), 'tp'), may hold values from -6 to 6
- mix_gain: float32 [2048], replicated, may hold values from 0.1 to 1.9
- w_u: bfloat16 [2048, 2048], P('fs', 'tp'), may hold values from -0.125 to 0.125
- w_v: bfloat16 [2048, 2048], P('fs', 'tp'), may hold values from -0.125 to 0.125
- norm_gain: float32 [2048], P('tp'), may hold values from 0.1 to 1.9
- mix_weight: bfloat16 [16, 128, 128], P('tp'), may hold values from -0.5 to 0.5
- mix_bias: float32 [16, 128], P('tp'), may hold values from 0.1 to 1.9
- w_mix_out: bfloat16 [2048, 2048], P('tp', 'fs'), may hold values from -0.125 to 0.125
- ffn_gain: float32 [2048], replicated, may hold values from 0.1 to 1.9
- w_gate: bfloat16 [2048, 3072], P('fs', 'tp'), may hold values from -0.125 to 0.125
- w_value: bfloat16 [2048, 3072], P('fs', 'tp'), may hold values from -0.125 to 0.125
- taps_gate: bfloat16 [3, 3072], P(None, 'tp'), may hold values from -3.5 to 3.5
- taps_value: bfloat16 [3, 3072], P(None, 'tp'), may hold values from -3.5 to 3.5
- w_down: bfloat16 [3072, 2048], P('tp', 'fs'), may hold values from -0.109375 to 0.109375
Outputs:
- layer_out: bfloat16 [6144, 2048], P(('rep', 'fs'), 'tp')
The draws below stay inside these ranges and needn't reach their ends.
All inputs are finite; a program needn't handle non-finite values.
Results may differ from the reference program's by a relative error of at most 0.017.
Values may be sent and summed in bfloat16 or wider, within the bound.
No kernel may reach another device: no remote copies, remote signals or barrier semaphores. Data moves between devices by JAX's collectives and lax.ppermute only.
A program may use at most 64 MiB of HBM per device.

```python
import jax
import jax.numpy as jnp
from jax import lax

D = 2048
GROUPS = 16
MIX_WIDTH = 2048
FF = 3072
BLOCK = 128
CONV = 3
TOK_DEV = 384
TOKENS = 6144
N_TP = 2


def level_of(rng, extent, split, low, top_value):
    level, own = 1.0, jax.random.fold_in(rng, 6)
    for dim, blocks in split:
        draws = jnp.exp(jax.random.uniform(jax.random.fold_in(own, dim), (blocks,), jnp.float32, low / len(split), top_value / len(split)))
        level = level * jnp.repeat(draws, extent[dim] // blocks).reshape([-1 if axis == dim else 1 for axis in range(len(extent))])
    return level


def scatter_about(own_key, extent, deviation, most, pieces=(), kind=jnp.bfloat16):
    drawn = jax.random.normal(own_key, extent, jnp.float32) * deviation
    if len(pieces) > 0:
        drawn = level_of(own_key, extent, pieces, -0.22, 0.18) * drawn
    return jnp.clip(drawn, min=-most, max=most).astype(kind)


def setup_inputs(seed: int = 0) -> dict:
    key_of = jax.random.split(jax.random.key(seed), 15)
    tokens = scatter_about(key_of[0], (TOKENS, D), 1.0, 6.0, ((0, 16), (1, 2)))
    mix_gain = jnp.clip(1.0 + 0.18 * jax.random.normal(key_of[1], (D,), jnp.float32), 0.1, 1.9)
    w_u = scatter_about(key_of[2], (D, MIX_WIDTH), D ** -0.5, 0.125, ((0, 8), (1, 2)))
    w_v = scatter_about(key_of[3], (D, MIX_WIDTH), D ** -0.5, 0.125, ((0, 8), (1, 2)))
    norm_gain = jnp.clip(1.0 + 0.18 * jax.random.normal(key_of[4], (MIX_WIDTH,), jnp.float32), 0.1, 1.9)
    mix_weight = scatter_about(key_of[5], (GROUPS, BLOCK, BLOCK), BLOCK ** -0.5, 0.5, ((0, 2),))
    mix_bias = jnp.clip(1.0 + 0.18 * jax.random.normal(key_of[6], (GROUPS, BLOCK), jnp.float32), 0.1, 1.9)
    w_mix_out = scatter_about(key_of[7], (MIX_WIDTH, D), MIX_WIDTH ** -0.5, 0.125, ((0, 2), (1, 8)))
    ffn_gain = jnp.clip(1.0 + 0.18 * jax.random.normal(key_of[8], (D,), jnp.float32), 0.1, 1.9)
    w_gate = scatter_about(key_of[9], (D, FF), D ** -0.5, 0.125, ((0, 8), (1, 2)))
    w_value = scatter_about(key_of[10], (D, FF), D ** -0.5, 0.125, ((0, 8), (1, 2)))
    taps_gate = scatter_about(key_of[11], (CONV, FF), CONV ** -0.5, 3.5, ((1, 2),))
    taps_value = scatter_about(key_of[12], (CONV, FF), CONV ** -0.5, 3.5, ((1, 2),))
    w_down = scatter_about(key_of[13], (FF, D), FF ** -0.5, 0.109375, ((0, 2), (1, 8)))
    return {"tokens": tokens, "mix_gain": mix_gain, "w_u": w_u, "w_v": w_v, "norm_gain": norm_gain, "mix_weight": mix_weight, "mix_bias": mix_bias, "w_mix_out": w_mix_out, "ffn_gain": ffn_gain, "w_gate": w_gate, "w_value": w_value, "taps_gate": taps_gate, "taps_value": taps_value, "w_down": w_down}


EPS_RMS = 1e-06
EPS_LN = 1e-05

def rms_scale(features, gain_vec):
    values = features.astype(jnp.float32)
    scaled = values * lax.rsqrt(lax.optimization_barrier(jnp.mean(values * values, axis=-1, keepdims=True)) + EPS_RMS)
    return (scaled * gain_vec).astype(jnp.bfloat16)

def spatial_mix(u_pre, v_pre, norm_gain, mix_weight, mix_bias):
    row_count = u_pre.shape[0]
    groups = mix_weight.shape[0]
    block_len = mix_weight.shape[1]
    group_width = v_pre.shape[1] // groups
    activated = jax.nn.gelu(v_pre).reshape(row_count, groups, group_width)
    average = lax.optimization_barrier(jnp.mean(activated, axis=-1, keepdims=True))
    spread_sq = lax.optimization_barrier(jnp.mean(jnp.square(activated - average), axis=-1, keepdims=True))
    v_norm = ((activated - average) * lax.rsqrt(spread_sq + EPS_LN) * norm_gain.reshape(groups, group_width)).astype(jnp.bfloat16)
    blocks = v_norm.reshape(row_count // block_len, block_len, groups, group_width)
    lower_mask = jnp.arange(block_len)[:, None] >= jnp.arange(block_len)[None, :]
    masked = jnp.where(lower_mask[None], mix_weight, jnp.zeros_like(mix_weight))
    mixed_rows = jnp.einsum('gts,nsgc->ntgc', masked.astype(jnp.float32), blocks.astype(jnp.float32))
    mixed_rows = mixed_rows + jnp.transpose(mix_bias)[None, :, :, None]
    mixed_rows = mixed_rows.reshape(row_count, groups * group_width)
    return (jax.nn.gelu(u_pre) * mixed_rows).astype(jnp.bfloat16)

def causal_taps(values, tap_weights, seq_len):
    row_count, channels = values.shape
    conv_len = tap_weights.shape[0]
    sequences = values.reshape(row_count // seq_len, seq_len, channels)
    padded = jnp.pad(sequences, ((0, 0), (conv_len - 1, 0), (0, 0)))
    summed_terms = jnp.zeros_like(sequences)
    for tap_index in range(conv_len):
        summed_terms = summed_terms + tap_weights[tap_index].astype(jnp.float32) * padded[:, tap_index:tap_index + seq_len]
    return summed_terms.reshape(row_count, channels)

def split_sum(operand, weight):
    share_width = operand.shape[1] // N_TP
    summed_terms = jnp.zeros((operand.shape[0], weight.shape[1]), jnp.float32)
    for member in range(N_TP):
        partial_value = jnp.dot(operand[:, member * share_width:(member + 1) * share_width], weight[member * share_width:(member + 1) * share_width], preferred_element_type=jnp.float32)
        rounded = lax.optimization_barrier(partial_value.astype(jnp.bfloat16))
        summed_terms = summed_terms + rounded.astype(jnp.float32)
    return summed_terms

def reference(tokens, mix_gain, w_u, w_v, norm_gain, mix_weight, mix_bias, w_mix_out, ffn_gain, w_gate, w_value, taps_gate, taps_value, w_down):
    normed = rms_scale(tokens, mix_gain)
    u_pre = jnp.dot(normed, w_u, preferred_element_type=jnp.float32)
    v_pre = jnp.dot(normed, w_v, preferred_element_type=jnp.float32)
    hidden = spatial_mix(u_pre, v_pre, norm_gain, mix_weight, mix_bias)
    middle = (tokens.astype(jnp.float32) + split_sum(hidden, w_mix_out)).astype(jnp.bfloat16)
    normed_mid = rms_scale(middle, ffn_gain)
    gate_pre = jnp.dot(normed_mid, w_gate, preferred_element_type=jnp.float32)
    value_pre = jnp.dot(normed_mid, w_value, preferred_element_type=jnp.float32)
    gate_conv = causal_taps(gate_pre, taps_gate, TOK_DEV)
    value_conv = causal_taps(value_pre, taps_value, TOK_DEV)
    activation = (jax.nn.gelu(gate_conv) * value_conv).astype(jnp.bfloat16)
    return (middle.astype(jnp.float32) + split_sum(activation, w_down)).astype(jnp.bfloat16)
```

```python
import jax
import jax.numpy as jnp
from jax import lax
from jax.sharding import PartitionSpec as P

EPS_RMS = 1e-06
EPS_LN = 1e-05


def swap(value, axis, size):
    return lax.ppermute(value, axis, [(i, i ^ 1) for i in range(size)])


def after(value, *others):
    return lax.optimization_barrier((value,) + others)[0]


def causal_taps(values, tap_weights):
    conv_len = tap_weights.shape[0]
    seq_len = values.shape[1]
    padded = jnp.pad(values, ((0, 0), (conv_len - 1, 0), (0, 0)))
    total = None
    for k in range(conv_len):
        term = tap_weights[k].astype(jnp.float32) * padded[:, k : k + seq_len]
        total = term if total is None else total + term
    return total


def build(sizes):
    reps, fs_count, tp_count = sizes["rep"], sizes["fs"], sizes["tp"]

    def on_device(
        tokens,
        mix_gain,
        w_u,
        w_v,
        norm_gain,
        mix_weight,
        mix_bias,
        w_mix_out,
        ffn_gain,
        w_gate,
        w_value,
        taps_gate,
        taps_value,
        w_down,
    ):
        groups = mix_weight.shape[0]
        block_len = mix_weight.shape[1]
        seq_len, own_width = tokens.shape
        width = own_width * tp_count
        split_r = reps == 2 and groups % 2 == 0
        split_y = fs_count % 2 == 0 and groups % (4 if split_r else 2) == 0
        r_parts, y_parts = (2 if split_r else 1), (2 if split_y else 1)
        parts = r_parts * y_parts
        z_count = fs_count // y_parts
        r_idx = lax.axis_index("rep") if split_r else 0
        f_idx = lax.axis_index("fs")
        t_idx = lax.axis_index("tp")
        y_idx = f_idx % y_parts
        z_idx = f_idx // y_parts
        part = r_idx * y_parts + y_idx
        part_y = r_idx * y_parts + (1 - y_idx)

        def swap_x(value):
            return swap(value, "rep", reps)

        def swap_y(value):
            return swap(value, "fs", fs_count)

        def z_perm(target):
            pairs = []
            for z in range(z_count):
                t = target(z)
                if t is not None:
                    for y in range(y_parts):
                        pairs.append((z * y_parts + y, t * y_parts + y))
            return pairs

        def shift(k):
            return z_perm(lambda z: z + k if 0 <= z + k < z_count else None)

        def gather_z(block):
            rows = block.shape[0]
            if z_count == 1:
                return block, block
            if z_count != 4:
                members = [
                    [z * y_parts + y for z in range(z_count)] for y in range(y_parts)
                ]
                full = lax.all_gather(block, "fs", axis=0, tiled=True, axis_index_groups=members)
                return full, full
            two = lax.ppermute(block, "fs", z_perm(lambda z: (z + 2) % 4))
            up = lax.ppermute(block, "fs", shift(1))
            down = lax.ppermute(block, "fs", shift(-1))
            relay = lax.ppermute(
                two, "fs", z_perm(lambda z: 3 if z == 2 else (0 if z == 1 else None))
            )
            one = jnp.where(z_idx == 0, relay, up)
            three = jnp.where(z_idx == 3, relay, down)
            full = jnp.zeros((4 * rows, block.shape[1]), block.dtype)
            for k, piece in enumerate((block, one, two, three)):
                full = lax.dynamic_update_slice_in_dim(full, piece, ((z_idx - k) % 4) * rows, 0)
            return full, two

        def cut_columns(weight, index):
            each = weight.shape[1] // parts
            return lax.dynamic_slice_in_dim(weight, index * each, each, 1)

        def cut_rows(weight, index):
            each = weight.shape[0] // parts
            return lax.dynamic_slice_in_dim(weight, index * each, each, 0).T

        def join_y(pieces_of):
            mine = jnp.concatenate(pieces_of(part), axis=1)
            if not split_y:
                return mine
            theirs = swap_y(jnp.concatenate(pieces_of(part_y), axis=1))
            low = jnp.where(y_idx == 0, mine, theirs)
            high = jnp.where(y_idx == 0, theirs, mine)
            return jnp.concatenate([low, high], axis=0)

        def uv_pieces(index):
            return [cut_columns(w_u, index), cut_columns(w_v, index)]

        def rest_pieces(index):
            return [
                cut_rows(w_mix_out, index),
                cut_columns(w_gate, index),
                cut_columns(w_value, index),
                cut_rows(w_down, index),
            ]

        mix_cols = w_u.shape[1] // parts
        ff_cols = w_gate.shape[1] // parts
        uv_block = join_y(uv_pieces)
        rest_block = join_y(rest_pieces)
        w_uv, uv_two = gather_z(uv_block)
        rest_block = after(rest_block, uv_two)
        w_mo_t, mo_two = gather_z(rest_block[:, :mix_cols])
        rest_block = after(rest_block, mo_two)
        w_gv, gv_two = gather_z(rest_block[:, mix_cols : mix_cols + 2 * ff_cols])
        rest_block = after(rest_block, gv_two)
        w_dn_t, _ = gather_z(rest_block[:, mix_cols + 2 * ff_cols :])

        def tp_other(value):
            return swap(value, "tp", tp_count)

        def gather_group(own):
            pieces = [own]
            if split_r:
                from_x = swap_x(own)
                pieces.append(from_x)
            if split_y:
                from_y = swap_y(own)
                pieces.append(from_y)
            if split_r and split_y:
                half = own.shape[1] // 2
                first = swap_x(from_y[:, :half])
                second = swap_y(from_x[:, half:])
                pieces.append(jnp.concatenate([first, second], axis=1))
            return jnp.stack(pieces)

        def gather_features(own):
            if tp_count == 2:
                other = tp_other(own)
                low = jnp.where(t_idx == 0, own, other)
                high = jnp.where(t_idx == 0, other, own)
                return jnp.concatenate([low, high], axis=-1)
            return lax.all_gather(own, "tp", axis=own.ndim - 1, tiled=True)

        def normalize(values, gain):
            wide = values.astype(jnp.float32)
            scale = lax.rsqrt(jnp.mean(wide * wide, axis=-1, keepdims=True) + EPS_RMS)
            return (wide * scale * gain).astype(jnp.bfloat16)

        def reduce_group(operand, weight_t):
            def product(cols_t):
                return lax.dot_general(
                    operand, cols_t, (((2,), (1,)), ((), ())), preferred_element_type=jnp.float32
                )

            if tp_count == 2:
                own_w = lax.dynamic_slice_in_dim(weight_t, t_idx * own_width, own_width, 0)
                other_w = lax.dynamic_slice_in_dim(weight_t, (1 - t_idx) * own_width, own_width, 0)
                other = tp_other(product(other_w).astype(jnp.bfloat16))
                total = product(own_w) + other.astype(jnp.float32)
            else:
                total = lax.psum_scatter(
                    product(weight_t).astype(jnp.bfloat16), "tp", scatter_dimension=2, tiled=True
                ).astype(jnp.float32)
            if not (split_r or split_y):
                return total[0]
            if not (split_r and split_y):
                mover = swap_x if split_r else swap_y
                return total[0] + mover(total[1].astype(jnp.bfloat16)).astype(jnp.float32)
            half = own_width // 2
            rows = total.shape[1]
            lo = total[:, :, :half]
            hi = total[:, :, half:]

            def send(mover, value):
                return mover(value.astype(jnp.bfloat16)).astype(jnp.float32)

            lo_in = send(swap_x, jnp.concatenate([lo[1], lo[3]], axis=0))
            hi_in = send(swap_y, jnp.concatenate([hi[2], hi[3]], axis=0))
            lo_fin = send(swap_y, lo[2] + lo_in[rows:])
            hi_fin = send(swap_x, hi[1] + hi_in[rows:])
            lo_sum = lo[0] + lo_in[:rows] + lo_fin
            hi_sum = hi[0] + hi_in[:rows] + hi_fin
            return jnp.concatenate([lo_sum, hi_sum], axis=1)

        features = gather_features(gather_group(tokens))
        normed = normalize(features, mix_gain)

        uv_pre = lax.dot_general(
            normed, w_uv, (((2,), (0,)), ((), ())), preferred_element_type=jnp.float32
        )
        u_pre, v_pre = uv_pre[..., :mix_cols], uv_pre[..., mix_cols:]

        my_groups = groups // parts
        gain = lax.dynamic_slice_in_dim(norm_gain, part * mix_cols, mix_cols, 0)
        mixers = lax.dynamic_slice_in_dim(mix_weight, part * my_groups, my_groups, 0)
        biases = lax.dynamic_slice_in_dim(mix_bias, part * my_groups, my_groups, 0)
        group_width = mix_cols // my_groups
        lower = jnp.arange(block_len)[:, None] >= jnp.arange(block_len)[None, :]
        mixers = jnp.where(lower[None], mixers, jnp.zeros_like(mixers))
        hidden_parts = []
        for g in range(my_groups):
            cols = slice(g * group_width, (g + 1) * group_width)
            act = jax.nn.gelu(v_pre[..., cols])
            average = jnp.mean(act, axis=-1, keepdims=True)
            spread = jnp.mean(jnp.square(act - average), axis=-1, keepdims=True)
            v_norm = ((act - average) * lax.rsqrt(spread + EPS_LN) * gain[cols]).astype(
                jnp.bfloat16
            )
            blocks = v_norm.reshape(-1, block_len, group_width)
            mixed = jnp.einsum("ts,nsc->ntc", mixers[g], blocks, preferred_element_type=jnp.float32)
            mixed = mixed + biases[g][None, :, None]
            mixed = mixed.reshape(parts, seq_len, group_width)
            hidden_parts.append((jax.nn.gelu(u_pre[..., cols]) * mixed).astype(jnp.bfloat16))
        hidden = jnp.concatenate(hidden_parts, axis=-1)

        mixer_sum = reduce_group(hidden, w_mo_t)
        middle = (tokens.astype(jnp.float32) + mixer_sum).astype(jnp.bfloat16)

        normed_mid = normalize(gather_features(gather_group(middle)), ffn_gain)
        gv_pre = lax.dot_general(
            normed_mid, w_gv, (((2,), (0,)), ((), ())), preferred_element_type=jnp.float32
        )
        tg = cut_columns(taps_gate, part)
        tv = cut_columns(taps_value, part)
        activation = (
            jax.nn.gelu(causal_taps(gv_pre[..., :ff_cols], tg))
            * causal_taps(gv_pre[..., ff_cols:], tv)
        ).astype(jnp.bfloat16)
        channel_sum = reduce_group(activation, w_dn_t)
        return (middle.astype(jnp.float32) + channel_sum).astype(jnp.bfloat16)

    return on_device


def solution(mesh):
    placed = (
        P(("rep", "fs"), "tp"),
        P(),
        P("fs", "tp"),
        P("fs", "tp"),
        P("tp"),
        P("tp", None, None),
        P("tp", None),
        P("tp", "fs"),
        P(),
        P("fs", "tp"),
        P("fs", "tp"),
        P(None, "tp"),
        P(None, "tp"),
        P("tp", "fs"),
    )
    return jax.shard_map(
        build(dict(mesh.shape)),
        mesh=mesh,
        in_specs=placed,
        out_specs=P(("rep", "fs"), "tp"),
        check_vma=False,
    )
```
